32 devices in a mesh: ep: 8 (over z, core), tp: 4 (over y, x).
Axes of the slice: x: 2, y: 2, z: 4, core: 2. Of those that a mesh axis runs over, the one named last changes fastest.
Arguments:
- mix_in: bfloat16 [2048, 2048], P('ep'), may hold values from -6 to 6
- mix_gain: float32 [2048], replicated, may hold values from 0.1 to 1.9
- w_in_x: bfloat16 [2048, 2048], P(None, 'tp'), may hold values from -0.125 to 0.125
- w_in_y: bfloat16 [2048, 2048], P(None, 'tp'), may hold values from -0.125 to 0.125
- conv_taps: float32 [4, 2048], P(None, 'tp'), may hold values from -3 to 3
- recur_gate_w: bfloat16 [16, 128, 128], P('tp'), may hold values from -0.5 to 0.5
- input_gate_w: bfloat16 [16, 128, 128], P('tp'), may hold values from -0.5 to 0.5
- decay_logit: float32 [2048], P('tp'), may hold values from 4 to 20
- decay_shift: float32 [2048, 2048], P('ep', 'tp'), may hold values from -2.2 to 0
- moe_in: bfloat16 [2048, 2048], P('ep'), may hold values from -6 to 6
- moe_gain: float32 [2048], replicated, may hold values from 0.1 to 1.9
- routes: int32 [2048, 2], P('ep'), may hold values from 0 to 7, all different within a row; in each aligned block of 256 rows (0 to 255, 256 to 511, ...) at most 128 rows name the same one
- route_weight: float32 [2048, 2], P('ep'), may hold values from 0.1 to 1
- expert_gate: bfloat16 [8, 2048, 2048], P('ep', None, 'tp'), may hold values from -0.125 to 0.125
- expert_up: bfloat16 [8, 2048, 2048], P('ep', None, 'tp'), may hold values from -0.125 to 0.125
- expert_down: bfloat16 [8, 2048, 2048], P('ep', None, 'tp'), may hold values from -0.125 to 0.125
Outputs:
- mixer_out: bfloat16 [2048, 2048], P('ep', 'tp')
- moe_out: bfloat16 [2048, 2048], P('ep', 'tp')
The draws below stay inside these ranges and needn't reach their ends.
Inputs may be any that keep to these rules, and one draw needn't show every extreme that they name: `routes`: each row names 2 different experts. Among the rows of one index of ep no expert is named more than 128 times, a bound that some block reaches.
All inputs are finite; a program needn't handle non-finite values.
Results may differ from the reference program's by a relative error of at most 0.0095.
Values may be sent and summed in bfloat16 or wider, within the bound.
A program may use at most 64 MiB of HBM per device.

```python
import math
import jax
import jax.numpy as jnp
import numpy as np
from jax import lax

D = 2048
FILTER_SECTIONS = 16
SECTION_FEATURES = 128
KCONV = 4
FF = 2048
TOPK = 2
TOK_DEV = 256
SUBBATCH_SPAN = 2048
WIDTH = 2048
EXPERTS = 8
CAP = 128
N_EP = 8


def draw_decay_logit(key, part):
    pick_key, slow_key, fast_key, jitter_key = jax.random.split(jax.random.fold_in(key, 11), 4)
    fast_head = jax.random.uniform(pick_key, (FILTER_SECTIONS,)) < 0.5
    slow_rate = jnp.exp(jax.random.uniform(slow_key, (FILTER_SECTIONS,), minval=math.log(0.2), maxval=math.log(0.6))) / SUBBATCH_SPAN
    fast_rate = jnp.exp(jax.random.uniform(fast_key, (FILTER_SECTIONS,), minval=math.log(0.01), maxval=math.log(1.0 / 30.0)))
    head_rate = jnp.where(fast_head, fast_rate, slow_rate)
    jitter = jax.random.uniform(jitter_key, (FILTER_SECTIONS, SECTION_FEATURES), minval=0.7, maxval=1.4)
    softened = (head_rate[:, None] * jitter / 4.0).reshape(FILTER_SECTIONS * SECTION_FEATURES)
    return -jnp.log(jnp.expm1(softened))


def draw_decay_shift(key, part):
    block_key, chan_key, place_key, depth_key = jax.random.split(jax.random.fold_in(key, 23), 4)
    blocks = SUBBATCH_SPAN // TOK_DEV
    spread = math.log(2.0)
    factor = jnp.exp(jax.random.uniform(block_key, (blocks,), minval=-spread, maxval=spread))
    channel = jax.random.uniform(chan_key, (FILTER_SECTIONS * SECTION_FEATURES,), minval=0.2, maxval=0.8)
    stationary_regime = -jnp.repeat(factor, TOK_DEV)[:, None] * channel[None, :] / SUBBATCH_SPAN
    assignment_seats = jax.random.randint(place_key, (3, FILTER_SECTIONS), 0, SUBBATCH_SPAN)
    stack_levels = jnp.log1p(-jax.random.uniform(depth_key, (3, FILTER_SECTIONS), minval=0.2, maxval=0.5))
    sequence_offsets = jnp.arange(SUBBATCH_SPAN)[:, None]
    packet_clusters = jnp.zeros((SUBBATCH_SPAN, FILTER_SECTIONS), jnp.float32)
    for picked_ordinal in range(3):
        packet_clusters = packet_clusters + jnp.where(sequence_offsets == assignment_seats[picked_ordinal][None, :], stack_levels[picked_ordinal][None, :], 0.0)
    return stationary_regime + jnp.repeat(packet_clusters, SECTION_FEATURES, axis=1)


def shard_levels(rng, shape, shards, least, high):
    factor_of = 1.0
    for axis_at, parts in shards:
        heights = jax.random.uniform(jax.random.fold_in(jax.random.fold_in(rng, 6), axis_at), (parts,), jnp.float32, least / len(shards), high / len(shards))
        factor_of = factor_of * jnp.repeat(jnp.exp(heights), shape[axis_at] // parts).reshape((-1,) + (1,) * (len(shape) - 1 - axis_at))
    return factor_of


def assign_block(rng, own, number, rows, amount, top, most, skew):
    sequence = jax.random.permutation(rng, amount)
    crowded, common = load_shares(amount, rows * top, most, skew, True), load_shares(amount, rows * top, most, skew, False)
    places = jnp.arange(amount)

    def named(sizes, offset_by):
        used = int((sizes > 0).sum())
        fixed = max(1, used // 4)
        passed = fixed + (places - fixed + offset_by * (used - fixed)) % max(1, amount - fixed)
        return jnp.zeros((amount,), jnp.int32).at[sequence[jnp.where(places < fixed, places, passed)]].set(jnp.asarray(sizes, jnp.int32))

    sizes = jnp.where(number % 4 == 0, named(crowded, number // 4), named(common, number - number // 4 - 1))
    mixed = jax.random.permutation(jax.random.fold_in(own, 3), amount)
    giver, taker = mixed[0:amount // 2 * 2:2], mixed[1:amount // 2 * 2:2]
    slack = jnp.minimum(sizes[giver] - 1, most - sizes[taker]) // 2
    slack = jnp.where((giver == sequence[0]) | (taker == sequence[0]) | (sizes[taker] == 0), 0, jnp.maximum(slack, 0))
    passed = jax.random.randint(jax.random.fold_in(own, 4), (amount // 2,), 0, 1 << 20) % (slack + 1)
    sizes = sizes.at[giver].add(-passed).at[taker].add(passed)
    labels = jnp.searchsorted(jnp.cumsum(sizes), jnp.arange(rows * top), side="right").astype(jnp.int32)
    listing = labels.reshape(top, rows).T
    listing = listing[jax.random.permutation(jax.random.fold_in(own, 1), rows)]
    offset_by = jax.random.randint(jax.random.fold_in(own, 2), (rows, 1), 0, top)
    return jnp.take_along_axis(listing, (jnp.arange(top)[None, :] + offset_by) % top, axis=1)


def load_shares(number_of, total, most, slope, full):
    portions = [(1 << 20) // math.isqrt(grade ** slope) + 1 for grade in range(1, number_of + 1)]
    largest = most if full else min(most, max(-(-total // number_of), total * portions[0] // sum(portions)))
    least = 1 if total - largest >= number_of - 1 else 0
    holding, spare = [largest] + [least] * (number_of - 1), total - largest - least * (number_of - 1)
    while spare > 0:
        free = [i for i in range(1, number_of) if holding[i] < largest] or [i for i in range(1, number_of) if holding[i] < most]
        mass, remaining = sum([portions[i] for i in free]), spare
        for i in free:
            more = min(most - holding[i], max(1, remaining * portions[i] // mass), spare)
            holding[i] = holding[i] + more
            spare = spare - more
    return np.array(holding)


def noise(rng, shape, scale, bound, shards=(), held_as=jnp.bfloat16):
    level = shard_levels(rng, shape, shards, -0.22, 0.18) if shards else 1.0
    drawn = jax.random.normal(rng, shape, jnp.float32) * scale * level
    return jnp.minimum(jnp.maximum(drawn, -bound), bound).astype(held_as)


def setup_inputs(seed: int = 0) -> dict:
    keys = jax.random.split(jax.random.key(seed), 17)
    mix_in = noise(keys[0], (SUBBATCH_SPAN, D), 1.0, 6.0, ((0, 8),))
    mix_gain = jnp.clip(1.0 + 0.18 * jax.random.normal(keys[1], (D,), jnp.float32), 0.1, 1.9)
    w_in_x = noise(keys[2], (D, WIDTH), D ** -0.5, 0.125, ((1, 4),))
    w_in_y = noise(keys[3], (D, WIDTH), D ** -0.5, 0.125, ((1, 4),))
    conv_taps = noise(keys[4], (KCONV, WIDTH), 0.5, 3.0, ((1, 4),), jnp.float32)
    recur_gate_w = noise(keys[5], (FILTER_SECTIONS, SECTION_FEATURES, SECTION_FEATURES), SECTION_FEATURES ** -0.5, 0.5, ((0, 4),))
    input_gate_w = noise(keys[6], (FILTER_SECTIONS, SECTION_FEATURES, SECTION_FEATURES), SECTION_FEATURES ** -0.5, 0.5, ((0, 4),))
    decay_logit = draw_decay_logit(jax.random.fold_in(keys[16], 71), 0)
    decay_shift = draw_decay_shift(jax.random.fold_in(keys[16], 71), 0)
    moe_in = noise(keys[9], (SUBBATCH_SPAN, D), 1.0, 6.0, ((0, 8),))
    moe_gain = jnp.clip(1.0 + 0.18 * jax.random.normal(keys[10], (D,), jnp.float32), 0.1, 1.9)
    routes_keys = jax.random.split(jax.random.fold_in(keys[11], 1), SUBBATCH_SPAN // TOK_DEV)
    routes_turns = jax.random.permutation(jax.random.fold_in(keys[11], 3), SUBBATCH_SPAN // TOK_DEV)
    routes = jax.vmap(lambda own, number: assign_block(jax.random.fold_in(keys[11], 2), own, number, TOK_DEV, EXPERTS, TOPK, CAP, 2))(routes_keys, routes_turns).reshape((SUBBATCH_SPAN, TOPK))
    route_weight = jnp.clip(jnp.exp(math.log(1.0) - 2.3025851 * jax.random.uniform(keys[12], (SUBBATCH_SPAN, TOPK), jnp.float32) ** shard_levels(keys[12], (SUBBATCH_SPAN, TOPK), ((0, 8),), -0.2, 0.2)), 0.1, 1.0)
    expert_gate = noise(keys[13], (EXPERTS, D, FF), D ** -0.5, 0.125, ((0, 8), (2, 4)))
    expert_up = noise(keys[14], (EXPERTS, D, FF), D ** -0.5, 0.125, ((0, 8), (2, 4)))
    expert_down = noise(keys[15], (EXPERTS, FF, D), FF ** -0.5, 0.125, ((0, 8), (2, 4)))
    return {"mix_in": mix_in, "mix_gain": mix_gain, "w_in_x": w_in_x, "w_in_y": w_in_y, "conv_taps": conv_taps, "recur_gate_w": recur_gate_w, "input_gate_w": input_gate_w, "decay_logit": decay_logit, "decay_shift": decay_shift, "moe_in": moe_in, "moe_gain": moe_gain, "routes": routes, "route_weight": route_weight, "expert_gate": expert_gate, "expert_up": expert_up, "expert_down": expert_down}


epsilon = 1e-06
lru_scale = 8.0

def norm_rows(rows, gain):
    widened = rows.astype(jnp.float32)
    scaled = widened * lax.rsqrt(lax.optimization_barrier(jnp.mean(widened * widened, axis=-1, keepdims=True)) + epsilon)
    return (scaled * gain.astype(jnp.float32)[None, :]).astype(jnp.bfloat16)

def link(earlier, later):
    return (earlier[0] * later[0], later[0] * earlier[1] + later[1])

def reference(mix_in, mix_gain, w_in_x, w_in_y, conv_taps, recur_gate_w, input_gate_w, decay_logit, decay_shift, moe_in, moe_gain, routes, route_weight, expert_gate, expert_up, expert_down):
    mixer_rows = norm_rows(mix_in, mix_gain)
    x_branch = jnp.dot(mixer_rows, w_in_x, preferred_element_type=jnp.float32).astype(jnp.bfloat16)
    y_branch = jnp.dot(mixer_rows, w_in_y, preferred_element_type=jnp.float32).astype(jnp.bfloat16)
    padded = jnp.concatenate([jnp.zeros((KCONV - 1, WIDTH), jnp.bfloat16), x_branch], axis=0)
    conv_sum = jnp.zeros((SUBBATCH_SPAN, WIDTH), jnp.float32)
    for tap_index in range(KCONV):
        conv_sum = conv_sum + conv_taps[tap_index][None, :].astype(jnp.float32) * padded[tap_index:tap_index + SUBBATCH_SPAN].astype(jnp.float32)
    x_conv = conv_sum.astype(jnp.bfloat16)
    heads_in = x_conv.astype(jnp.float32).reshape(SUBBATCH_SPAN, FILTER_SECTIONS, SECTION_FEATURES)
    gate_a = jnp.einsum('thi,hij->thj', heads_in, recur_gate_w.astype(jnp.float32)).reshape(SUBBATCH_SPAN, WIDTH)
    gate_x = jnp.einsum('thi,hij->thj', heads_in, input_gate_w.astype(jnp.float32)).reshape(SUBBATCH_SPAN, WIDTH)
    log_decay = -lru_scale * jax.nn.sigmoid(gate_a) * jax.nn.softplus(-decay_logit)[None, :] + decay_shift
    lru_drive = jnp.sqrt(-jnp.expm1(2.0 * log_decay)) * jax.nn.sigmoid(gate_x) * x_conv.astype(jnp.float32)
    through, lru_state = lax.associative_scan(link, (jnp.exp(log_decay), lru_drive), axis=0)
    mixer_out = (lru_state * jax.nn.gelu(y_branch.astype(jnp.float32))).astype(jnp.bfloat16)
    moe_rows = norm_rows(moe_in, moe_gain)
    grouped = routes.reshape(N_EP, TOK_DEV * TOPK)
    onehot = (grouped[:, :, None] == jnp.arange(EXPERTS, dtype=jnp.int32)[None, None, :]).astype(jnp.int32)
    slot_rank = lax.optimization_barrier(jnp.sum(jnp.cumsum(onehot, axis=1) * onehot, axis=2)) - 1
    source = jnp.broadcast_to(jnp.arange(N_EP, dtype=jnp.int32)[:, None], slot_rank.shape)
    slot_index = (source * CAP + slot_rank).reshape(-1).astype(jnp.int32)
    expert_ids = routes.reshape(-1).astype(jnp.int32)
    token_index = jnp.repeat(jnp.arange(SUBBATCH_SPAN, dtype=jnp.int32), TOPK)
    table = jnp.zeros((EXPERTS, N_EP * CAP, D), jnp.bfloat16).at[expert_ids, slot_index].set(moe_rows[token_index])

    def run_expert(packed):
        rows_in, gate_w, up_w, down_w = packed
        gate_proj = jnp.dot(rows_in, gate_w, preferred_element_type=jnp.float32)
        up_proj = jnp.dot(rows_in, up_w, preferred_element_type=jnp.float32)
        hidden = (jax.nn.silu(gate_proj) * up_proj).astype(jnp.bfloat16)
        return jnp.dot(hidden, down_w, preferred_element_type=jnp.float32).astype(jnp.bfloat16)
    results = lax.map(run_expert, (table, expert_gate, expert_up, expert_down))
    picked = results[expert_ids, slot_index].astype(jnp.float32).reshape(SUBBATCH_SPAN, TOPK, D)
    route_share = route_weight / lax.optimization_barrier(jnp.sum(route_weight, axis=1, keepdims=True))
    moe_out = lax.optimization_barrier(jnp.sum(route_share[:, :, None] * picked, axis=1)).astype(jnp.bfloat16)
    return (mixer_out, moe_out)
```

```python
import functools

import jax
import jax.numpy as jnp
from jax import lax
from jax.experimental import pallas as pl
from jax.experimental.pallas import tpu as pltpu
from jax.sharding import PartitionSpec as P

epsilon = 1e-06
lru_scale = 8.0
MESH = pl.DeviceIdType.MESH
F32 = jnp.float32
BF16 = jnp.bfloat16


def near_first(count):
    return [sorted(range(count), key=lambda q: (abs(q - z), -q)) for z in range(count)]


def moe_kernel(
    cap,
    moe_hbm,
    gain_ref,
    rt_row,
    rt_col,
    rw_col,
    gate_hbm,
    up_hbm,
    down_hbm,
    out_ref,
    tok,
    hid,
    xs,
    res,
    ret,
    routes_all,
    gw,
    uw,
    dw,
    load_sem,
    rt_sem,
    z_send,
    z_recv,
    t_sem,
    sib_sem,
    own_sem,
    h_sem,
    ret_sem,
):
    n_ep = lax.axis_size("ep")
    nz = n_ep // 2
    ep = lax.axis_index("ep")
    t = lax.axis_index("tp")
    z, c = ep // 2, ep % 2
    y, x = t // 2, t % 2
    xp, yp, dg = y * 2 + (1 - x), (1 - y) * 2 + x, 3 - t
    rows, share = tok.shape[3], tok.shape[4]
    half = rows // 2
    pair = 2 * cap
    pair_half = pair // 2
    sibling = {"ep": z * 2 + (1 - c)}
    table = near_first(nz)

    def block_at(s):
        q = jnp.int32(0)
        for zz in range(nz):
            for ss in range(nz):
                q = jnp.where((z == zz) & (s == ss), table[zz][ss], q)
        return q

    def remote(src, dst, send, recv, where):
        return pltpu.make_async_remote_copy(
            src_ref=src,
            dst_ref=dst,
            send_sem=send,
            recv_sem=recv,
            device_id=where,
            device_id_type=MESH,
        )

    loads = [
        pltpu.make_async_copy(
            moe_hbm.at[:, pl.ds(k * share, share)], tok.at[c, z, k], load_sem.at[k]
        )
        for k in range(4)
    ] + [
        pltpu.make_async_copy(gate_hbm.at[0], gw, load_sem.at[4]),
        pltpu.make_async_copy(up_hbm.at[0], uw, load_sem.at[5]),
        pltpu.make_async_copy(down_hbm.at[0], dw, load_sem.at[6]),
    ]
    for copy in loads:
        copy.start()

    barrier = pltpu.get_barrier_semaphore()
    for by in range(1, n_ep):
        pl.semaphore_signal(
            barrier, inc=1, device_id={"ep": (ep + by) % n_ep}, device_id_type=MESH
        )
    for peer in (xp, yp):
        pl.semaphore_signal(barrier, inc=1, device_id={"tp": peer}, device_id_type=MESH)
    pl.semaphore_wait(barrier, n_ep + 1)

    def route_copy(by):
        return remote(
            rt_row,
            routes_all.at[ep],
            rt_sem.at[0, by],
            rt_sem.at[1, ep],
            {"ep": (ep + by) % n_ep},
        )

    for by in range(1, n_ep):
        route_copy(by).start()
    routes_all[ep] = rt_row[...]

    def z_copy(q, up):
        return remote(
            tok.at[c, q, t],
            tok.at[c, q, t],
            z_send.at[up, q],
            z_recv.at[q],
            {"ep": ep + (2 if up else -2)},
        )

    def t_copy(q, kind):
        if kind == 0:
            part, where = tok.at[c, q, t], {"tp": xp}
        elif kind == 1:
            part, where = tok.at[c, q, t], {"tp": yp}
        elif kind == 2:
            part, where = tok.at[c, q, yp, pl.ds(half, half)], {"tp": xp}
        else:
            part, where = tok.at[c, q, xp, pl.ds(0, half)], {"tp": yp}
        return remote(part, part, t_sem.at[0, kind, q], t_sem.at[1, kind, q], where)

    def sib_copy(q, k):
        part = tok.at[c, q, k]
        return remote(part, part, sib_sem.at[0, k, q], sib_sem.at[1, k, q], sibling)

    def own_copy():
        part = tok.at[c, z]
        return remote(part, part, own_sem.at[0], own_sem.at[1], sibling)

    def h_copy(q, kind):
        if kind == 0:
            part, where = hid.at[q, t], {"tp": xp}
        elif kind == 1:
            part, where = hid.at[q, t], {"tp": yp}
        elif kind == 2:
            part, where = hid.at[q, yp, pl.ds(pair_half, pair_half)], {"tp": xp}
        else:
            part, where = hid.at[q, xp, pl.ds(0, pair_half)], {"tp": yp}
        return remote(part, part, h_sem.at[0, kind, q], h_sem.at[1, kind, q], where)

    def ret_copy(q, cc):
        part = res.at[q * 2 + cc]
        return remote(
            part, ret.at[ep], ret_sem.at[0, q * 2 + cc], ret_sem.at[1, ep], {"ep": q * 2 + cc}
        )

    def spread(q):
        t_copy(q, 0).start()
        t_copy(q, 1).start()

        @pl.when((q < z) & (z + 1 < nz))
        def _():
            z_copy(q, 1).start()

        @pl.when((q > z) & (z > 0))
        def _():
            z_copy(q, 0).start()

        sib_copy(q, t).start()

    def ranks_row(block):
        named = routes_all[block]
        mask = jnp.where((named[0:1] == ep) | (named[1:2] == ep), 1.0, 0.0)
        before = jnp.where(
            lax.broadcasted_iota(jnp.int32, (rows, rows), 0)
            < lax.broadcasted_iota(jnp.int32, (rows, rows), 1),
            1.0,
            0.0,
        ).astype(BF16)
        rank = jnp.dot(
            jnp.broadcast_to(mask, (8, rows)).astype(BF16), before, preferred_element_type=F32
        )[0:1]
        key = jnp.where(mask > 0.5, rank, -1.0)
        seat = lax.broadcasted_iota(jnp.int32, (cap, rows), 0).astype(F32)
        return jnp.where(seat == key, 1.0, 0.0).astype(BF16)

    def expert_in(q):
        for cc in range(2):
            pick = ranks_row(q * 2 + cc)
            parts = [
                jnp.dot(pick, tok[cc, q, k], preferred_element_type=F32) for k in range(4)
            ]
            square = sum(jnp.sum(part * part, axis=-1, keepdims=True) for part in parts)
            scale = lax.rsqrt(square * (1.0 / (4 * share)) + epsilon)
            for k in range(4):
                xs[pl.ds(cc * cap, cap), pl.ds(k * share, share)] = (
                    parts[k] * scale * gain_ref[:, pl.ds(k * share, share)]
                ).astype(BF16)

        tile = 256

        @pl.loop(0, gw.shape[1] // tile)
        def _(j):
            cols = pl.ds(pl.multiple_of(j * tile, tile), tile)
            g = jnp.dot(xs[...], gw[:, cols], preferred_element_type=F32)
            u = jnp.dot(xs[...], uw[:, cols], preferred_element_type=F32)
            hid[q, t, :, cols] = (jax.nn.silu(g) * u).astype(BF16)

        h_copy(q, 0).start()
        h_copy(q, 1).start()

    def expert_out(q):
        tile = 256
        span = hid.shape[3]

        @pl.loop(0, dw.shape[1] // tile)
        def _(j):
            cols = pl.ds(pl.multiple_of(j * tile, tile), tile)
            total = jnp.zeros((pair, tile), F32)
            for k in range(4):
                total = total + jnp.dot(
                    hid[q, k], dw[pl.ds(k * span, span), cols], preferred_element_type=F32
                )
            out = total.astype(BF16)
            res[q * 2, :, cols] = out[:cap]
            res[q * 2 + 1, :, cols] = out[cap:]

        for cc in range(2):
            mine = (q == z) & (c == cc)

            @pl.when(jnp.logical_not(mine))
            def _():
                ret_copy(q, cc).start()

            @pl.when(mine)
            def _():
                ret[ep] = res[q * 2 + cc]

    for k in range(4):
        loads[k].wait()

    @pl.when(z + 1 < nz)
    def _():
        z_copy(z, 1).start()

    @pl.when(z > 0)
    def _():
        z_copy(z, 0).start()

    own_copy().start()
    for k in range(4, 7):
        loads[k].wait()
    for by in range(1, n_ep):
        other = (ep + by) % n_ep
        remote(
            rt_row, routes_all.at[other], rt_sem.at[0, 0], rt_sem.at[1, other], {"ep": other}
        ).wait_recv()
    remote(
        tok.at[1 - c, z], tok.at[1 - c, z], own_sem.at[0], own_sem.at[1], sibling
    ).wait_recv()
    expert_in(z)
    first = block_at(1)
    z_copy(first, 1).wait_recv()
    spread(first)

    def step(s, carry):
        q = block_at(s)
        nxt = block_at(s + 1)
        far = block_at(s + 2)
        h_copy(q, 0).wait_recv()
        h_copy(q, 3).start()
        h_copy(q, 1).wait_recv()
        h_copy(q, 2).start()

        @pl.when(s + 1 < nz)
        def _():
            t_copy(nxt, 0).wait_recv()
            t_copy(nxt, 3).start()
            sib_copy(nxt, xp).start()
            t_copy(nxt, 1).wait_recv()
            t_copy(nxt, 2).start()
            sib_copy(nxt, yp).start()

            @pl.when(s + 2 < nz)
            def _():
                z_copy(far, 1).wait_recv()
                spread(far)

            t_copy(nxt, 2).wait_recv()
            t_copy(nxt, 3).wait_recv()
            sib_copy(nxt, dg).start()
            for k in range(4):
                sib_copy(nxt, k).wait_recv()
            expert_in(nxt)

        h_copy(q, 2).wait_recv()
        h_copy(q, 3).wait_recv()
        expert_out(q)
        return carry

    lax.fori_loop(0, nz, step, 0)

    one, two = rt_col[:, 0:1], rt_col[:, 1:2]
    lane = lax.broadcasted_iota(jnp.int32, (rows, 128), 1)
    mask = jnp.where((one == lane) | (two == lane), 1.0, 0.0)
    before = jnp.where(
        lax.broadcasted_iota(jnp.int32, (rows, rows), 1)
        < lax.broadcasted_iota(jnp.int32, (rows, rows), 0),
        1.0,
        0.0,
    ).astype(BF16)
    rank = jnp.dot(before, mask.astype(BF16), preferred_element_type=F32)
    key = jnp.where(mask > 0.5, rank, -1.0)
    total_weight = rw_col[:, 0:1] + rw_col[:, 1:2]
    part_one = rw_col[:, 0:1] / total_weight
    part_two = rw_col[:, 1:2] / total_weight
    seat = lax.broadcasted_iota(jnp.int32, (rows, cap), 1).astype(F32)
    for by in range(1, n_ep):
        other = (ep + by) % n_ep
        remote(
            res.at[other], ret.at[other], ret_sem.at[0, other], ret_sem.at[1, other], {"ep": other}
        ).wait_recv()
    total = jnp.zeros((rows, ret.shape[2]), F32)
    for e in range(n_ep):
        pick = jnp.where(seat == key[:, e : e + 1], 1.0, 0.0).astype(BF16)
        portion = jnp.where(one == e, part_one, 0.0) + jnp.where(two == e, part_two, 0.0)
        total = total + portion * jnp.dot(pick, ret[e], preferred_element_type=F32)
    out_ref[...] = total.astype(BF16)

    for by in range(1, n_ep):
        route_copy(by).wait_send()

    @pl.when(z + 1 < nz)
    def _():
        z_copy(z, 1).wait_send()

    @pl.when(z > 0)
    def _():
        z_copy(z, 0).wait_send()

    own_copy().wait_send()

    def drain(q, carry):
        for kind in range(4):
            h_copy(q, kind).wait_send()

        @pl.when(q != z)
        def _():
            for kind in range(4):
                t_copy(q, kind).wait_send()
                sib_copy(q, kind).wait_send()

        @pl.when((q < z) & (z + 1 < nz))
        def _():
            z_copy(q, 1).wait_send()

        @pl.when((q > z) & (z > 0))
        def _():
            z_copy(q, 0).wait_send()

        for cc in range(2):

            @pl.when((q != z) | (c != cc))
            def _():
                ret_copy(q, cc).wait_send()

        return carry

    lax.fori_loop(0, nz, drain, 0)


def moe_fused(moe_in, moe_gain, routes, route_weight, expert_gate, expert_up, expert_down):
    n_ep = lax.axis_size("ep")
    nz = n_ep // 2
    rows, features = moe_in.shape
    share = features // 4
    ff_dev, out_dev = expert_gate.shape[2], expert_down.shape[2]
    cap = 2 * rows * routes.shape[1] // n_ep
    vmem = pl.BlockSpec(memory_space=pltpu.VMEM)
    anywhere = pl.BlockSpec(memory_space=pl.ANY)
    dma = pltpu.SemaphoreType.DMA
    flops = 2 * n_ep * cap * features * (2 * ff_dev + out_dev)
    return pl.pallas_call(
        functools.partial(moe_kernel, cap),
        out_shape=jax.ShapeDtypeStruct((rows, out_dev), BF16),
        in_specs=[anywhere, vmem, vmem, vmem, vmem, anywhere, anywhere, anywhere],
        out_specs=vmem,
        scratch_shapes=[
            pltpu.VMEM((2, nz, 4, rows, share), BF16),
            pltpu.VMEM((nz, 4, 2 * cap, ff_dev), BF16),
            pltpu.VMEM((2 * cap, features), BF16),
            pltpu.VMEM((n_ep, cap, out_dev), BF16),
            pltpu.VMEM((n_ep, cap, out_dev), BF16),
            pltpu.VMEM((n_ep, 2, rows), jnp.int32),
            pltpu.VMEM(expert_gate.shape[1:], BF16),
            pltpu.VMEM(expert_up.shape[1:], BF16),
            pltpu.VMEM(expert_down.shape[1:], BF16),
            dma((7,)),
            dma((2, n_ep)),
            dma((2, nz)),
            dma((nz,)),
            dma((2, 4, nz)),
            dma((2, 4, nz)),
            dma((2,)),
            dma((2, 4, nz)),
            dma((2, n_ep)),
        ],
        compiler_params=pltpu.CompilerParams(
            collective_id=0, has_side_effects=True, vmem_limit_bytes=48 * 1024 * 1024
        ),
        cost_estimate=pl.CostEstimate(flops=flops, bytes_accessed=8 << 20, transcendentals=0),
        name="moe",
    )(
        moe_in,
        moe_gain[None, :],
        routes.T,
        routes,
        route_weight,
        expert_gate,
        expert_up,
        expert_down,
    )


def from_behind(value, axis, by):
    count = lax.axis_size(axis)
    pairs = [(i, i + by) for i in range(count) if 0 <= i + by < count]
    return lax.ppermute(value, axis, pairs)


def entering(value, axis, combine, identity):
    count, index = (lax.axis_size(axis), lax.axis_index(axis))
    everything = jax.tree.map(lambda part: lax.all_gather(part, axis), value)
    start = jax.tree.map(
        lambda part, zero: jnp.broadcast_to(jnp.asarray(zero, part.dtype), part.shape),
        value,
        identity,
    )

    def hop(k, before):
        reached = k < index
        new = combine(before, jax.tree.map(lambda part: part[k], everything))
        return jax.tree.map(lambda a, b: jnp.where(reached, a, b), new, before)

    return lax.fori_loop(0, count, hop, start)


def norm_rows(rows, gain):
    widened = rows.astype(jnp.float32)
    scaled = widened * lax.rsqrt(jnp.mean(widened * widened, axis=-1, keepdims=True) + epsilon)
    return (scaled * gain[None, :]).astype(jnp.bfloat16)


def link(earlier, later):
    return (earlier[0] * later[0], later[0] * earlier[1] + later[1])


def fits_fused(moe_in):
    gathered = lax.axis_size("ep") * moe_in.size * moe_in.dtype.itemsize
    return lax.axis_size("tp") == 4 and gathered <= (16 << 20)


def moe_staged(moe_in, moe_gain, routes, route_weight, expert_gate, expert_up, expert_down):
    moe_rows = norm_rows(moe_in, moe_gain)
    token_count = moe_rows.shape[0]
    feature_count = moe_rows.shape[1]
    choose_count = routes.shape[1]
    expert_count = lax.axis_size("ep")
    capacity = 2 * token_count * choose_count // expert_count
    slot_total = expert_count * capacity
    expert_ids = routes.reshape(-1)
    onehot = (expert_ids[:, None] == jnp.arange(expert_count, dtype=jnp.int32)[None, :]).astype(
        jnp.int32
    )
    slot_rank = jnp.sum(jnp.cumsum(onehot, axis=0) * onehot, axis=1) - 1
    slot_index = expert_ids * capacity + slot_rank
    token_index = jnp.repeat(jnp.arange(token_count, dtype=jnp.int32), choose_count)
    slot_owner = jnp.full((slot_total,), token_count, jnp.int32).at[slot_index].set(token_index)
    padded_rows = jnp.concatenate([moe_rows, jnp.zeros((1, feature_count), jnp.bfloat16)], axis=0)
    outgoing = padded_rows[slot_owner].reshape(expert_count, capacity, feature_count)
    column_width = feature_count // lax.axis_size("tp")
    own_columns = lax.dynamic_slice_in_dim(
        outgoing, lax.axis_index("tp") * column_width, column_width, 2
    )
    incoming = lax.all_to_all(own_columns, "ep", split_axis=0, concat_axis=0, tiled=True)
    piece = lax.all_gather(incoming, "tp", axis=2, tiled=True)
    flat_rows = piece.reshape(slot_total, piece.shape[2])
    gate_rows = expert_gate[0]
    up_rows = expert_up[0]
    gate_proj = jnp.dot(flat_rows, gate_rows, preferred_element_type=jnp.float32)
    up_proj = jnp.dot(flat_rows, up_rows, preferred_element_type=jnp.float32)
    hidden = (jax.nn.silu(gate_proj) * up_proj).astype(jnp.bfloat16)
    down_rows = expert_down[0]
    columns = jnp.dot(
        lax.all_gather(hidden, "tp", axis=1, tiled=True),
        down_rows,
        preferred_element_type=jnp.float32,
    )
    results = columns.astype(jnp.bfloat16).reshape(expert_count, capacity, expert_down.shape[2])
    returned = lax.all_to_all(results, "ep", split_axis=0, concat_axis=0, tiled=True).reshape(
        slot_total, expert_down.shape[2]
    )
    picked = (
        returned[slot_index]
        .astype(jnp.float32)
        .reshape(token_count, choose_count, expert_down.shape[2])
    )
    route_share = route_weight / jnp.sum(route_weight, axis=1, keepdims=True)
    moe_out = jnp.sum(route_share[:, :, None] * picked, axis=1).astype(jnp.bfloat16)
    return moe_out


def local(
    mix_in,
    mix_gain,
    w_in_x,
    w_in_y,
    conv_taps,
    recur_gate_w,
    input_gate_w,
    decay_logit,
    decay_shift,
    moe_in,
    moe_gain,
    routes,
    route_weight,
    expert_gate,
    expert_up,
    expert_down,
):
    row_count = mix_in.shape[0]
    width_dev = w_in_x.shape[1]
    heads_dev = recur_gate_w.shape[0]
    block_size = recur_gate_w.shape[1]
    tap_count = conv_taps.shape[0]
    mixer_rows = norm_rows(mix_in, mix_gain)
    x_branch = jnp.dot(mixer_rows, w_in_x, preferred_element_type=jnp.float32).astype(jnp.bfloat16)
    y_branch = jnp.dot(mixer_rows, w_in_y, preferred_element_type=jnp.float32).astype(jnp.bfloat16)
    previous = from_behind(x_branch[row_count - (tap_count - 1) :], "ep", 1)
    padded = jnp.concatenate([previous, x_branch], axis=0)
    conv_sum = jnp.zeros((row_count, width_dev), jnp.float32)
    for tap_index in range(tap_count):
        conv_sum = conv_sum + conv_taps[tap_index][None, :] * padded[
            tap_index : tap_index + row_count
        ].astype(jnp.float32)
    x_conv = conv_sum.astype(jnp.bfloat16)
    heads_in = x_conv.reshape(row_count, heads_dev, block_size)
    gate_a = jnp.einsum(
        "thi,hij->thj", heads_in, recur_gate_w, preferred_element_type=jnp.float32
    ).reshape(row_count, width_dev)
    gate_x = jnp.einsum(
        "thi,hij->thj", heads_in, input_gate_w, preferred_element_type=jnp.float32
    ).reshape(row_count, width_dev)
    log_decay = (
        -lru_scale * jax.nn.sigmoid(gate_a) * jax.nn.softplus(-decay_logit)[None, :] + decay_shift
    )
    lru_drive = (
        jnp.sqrt(-jnp.expm1(2.0 * log_decay)) * jax.nn.sigmoid(gate_x) * x_conv.astype(jnp.float32)
    )
    through, local_state = lax.associative_scan(link, (jnp.exp(log_decay), lru_drive), axis=0)
    identity = (jnp.ones((width_dev,), jnp.float32), jnp.zeros((width_dev,), jnp.float32))
    carried = entering((through[row_count - 1], local_state[row_count - 1]), "ep", link, identity)
    lru_state = local_state + through * carried[1][None, :]
    mixer_out = (lru_state * jax.nn.gelu(y_branch.astype(jnp.float32))).astype(jnp.bfloat16)
    moe_args = (moe_in, moe_gain, routes, route_weight, expert_gate, expert_up, expert_down)
    moe_out = (moe_fused if fits_fused(moe_in) else moe_staged)(*moe_args)
    return (mixer_out, moe_out)


def solution(mesh):
    placed = (
        P("ep", None),
        P(),
        P(None, "tp"),
        P(None, "tp"),
        P(None, "tp"),
        P("tp", None, None),
        P("tp", None, None),
        P("tp"),
        P("ep", "tp"),
        P("ep", None),
        P(),
        P("ep", None),
        P("ep", None),
        P("ep", None, "tp"),
        P("ep", None, "tp"),
        P("ep", None, "tp"),
    )
    return jax.shard_map(
        local, mesh=mesh, in_specs=placed, out_specs=(P("ep", "tp"), P("ep", "tp")), check_vma=False
    )
```

```python
import functools

import jax
import jax.numpy as jnp
from jax import lax
from jax.experimental import pallas as pl
from jax.experimental.pallas import tpu as pltpu
from jax.sharding import PartitionSpec as P

epsilon = 1e-06
lru_scale = 8.0
MESH = pl.DeviceIdType.MESH
F32 = jnp.float32
BF16 = jnp.bfloat16


def near_first(count):
    return [sorted(range(count), key=lambda q: (abs(q - z), -q)) for z in range(count)]


def one_minus_exp(value):
    series = jnp.full_like(value, 1.0 / 9.0)
    for k in range(8, 1, -1):
        series = (1.0 + value * series) * (1.0 / k)
    series = 1.0 + value * series
    return jnp.where(value > -0.5, -value * series, 1.0 - jnp.exp(value))


def both_kernel(
    cap,
    mix_hbm,
    wx_hbm,
    wy_hbm,
    ga_hbm,
    gx_hbm,
    shift_hbm,
    mix_gain_ref,
    taps_ref,
    soft_ref,
    moe_hbm,
    gain_ref,
    rt_row,
    rt_col,
    rw_col,
    gate_hbm,
    up_hbm,
    down_hbm,
    mix_ref,
    out_ref,
    tok,
    hid,
    xs,
    res,
    ret,
    routes_all,
    gw,
    uw,
    dw,
    load_sem,
    rt_sem,
    z_send,
    z_recv,
    t_sem,
    sib_sem,
    own_sem,
    h_sem,
    ret_sem,
    mixv,
    wx,
    wy,
    gaw,
    gxw,
    shiftv,
    xb,
    yb,
    av,
    bv,
    ends,
    halo_sem,
    ends_sem,
):
    n_ep = lax.axis_size("ep")
    nz = n_ep // 2
    ep = lax.axis_index("ep")
    t = lax.axis_index("tp")
    z, c = ep // 2, ep % 2
    y, x = t // 2, t % 2
    xp, yp, dg = y * 2 + (1 - x), (1 - y) * 2 + x, 3 - t
    rows, share = tok.shape[3], tok.shape[4]
    half = rows // 2
    pair = 2 * cap
    pair_half = pair // 2
    sibling = {"ep": z * 2 + (1 - c)}
    table = near_first(nz)

    def block_at(s):
        q = jnp.int32(0)
        for zz in range(nz):
            for ss in range(nz):
                q = jnp.where((z == zz) & (s == ss), table[zz][ss], q)
        return q

    def remote(src, dst, send, recv, where):
        return pltpu.make_async_remote_copy(
            src_ref=src,
            dst_ref=dst,
            send_sem=send,
            recv_sem=recv,
            device_id=where,
            device_id_type=MESH,
        )

    loads = [
        pltpu.make_async_copy(
            moe_hbm.at[:, pl.ds(k * share, share)], tok.at[c, z, k], load_sem.at[k]
        )
        for k in range(4)
    ] + [
        pltpu.make_async_copy(gate_hbm.at[0], gw, load_sem.at[4]),
        pltpu.make_async_copy(up_hbm.at[0], uw, load_sem.at[5]),
        pltpu.make_async_copy(mix_hbm, mixv, load_sem.at[6]),
        pltpu.make_async_copy(wx_hbm, wx, load_sem.at[7]),
        pltpu.make_async_copy(wy_hbm, wy, load_sem.at[8]),
        pltpu.make_async_copy(ga_hbm, gaw, load_sem.at[9]),
        pltpu.make_async_copy(gx_hbm, gxw, load_sem.at[10]),
        pltpu.make_async_copy(shift_hbm, shiftv, load_sem.at[11]),
        pltpu.make_async_copy(down_hbm.at[0], dw, load_sem.at[12]),
    ]
    for copy in loads:
        copy.start()

    barrier = pltpu.get_barrier_semaphore()
    for by in range(1, n_ep):
        pl.semaphore_signal(
            barrier, inc=1, device_id={"ep": (ep + by) % n_ep}, device_id_type=MESH
        )
    for peer in (xp, yp):
        pl.semaphore_signal(barrier, inc=1, device_id={"tp": peer}, device_id_type=MESH)
    pl.semaphore_wait(barrier, n_ep + 1)

    def route_copy(by):
        return remote(
            rt_row,
            routes_all.at[ep],
            rt_sem.at[0, by],
            rt_sem.at[1, ep],
            {"ep": (ep + by) % n_ep},
        )

    for by in range(1, n_ep):
        route_copy(by).start()
    routes_all[ep] = rt_row[...]

    def z_copy(q, up):
        return remote(
            tok.at[c, q, t],
            tok.at[c, q, t],
            z_send.at[up, q],
            z_recv.at[q],
            {"ep": ep + (2 if up else -2)},
        )

    def t_copy(q, kind):
        if kind == 0:
            part, where = tok.at[c, q, t], {"tp": xp}
        elif kind == 1:
            part, where = tok.at[c, q, t], {"tp": yp}
        elif kind == 2:
            part, where = tok.at[c, q, yp, pl.ds(half, half)], {"tp": xp}
        else:
            part, where = tok.at[c, q, xp, pl.ds(0, half)], {"tp": yp}
        return remote(part, part, t_sem.at[0, kind, q], t_sem.at[1, kind, q], where)

    def sib_copy(q, k):
        part = tok.at[c, q, k]
        return remote(part, part, sib_sem.at[0, k, q], sib_sem.at[1, k, q], sibling)

    def own_copy():
        part = tok.at[c, z]
        return remote(part, part, own_sem.at[0], own_sem.at[1], sibling)

    def h_copy(q, kind):
        if kind == 0:
            part, where = hid.at[q, t], {"tp": xp}
        elif kind == 1:
            part, where = hid.at[q, t], {"tp": yp}
        elif kind == 2:
            part, where = hid.at[q, yp, pl.ds(pair_half, pair_half)], {"tp": xp}
        else:
            part, where = hid.at[q, xp, pl.ds(0, pair_half)], {"tp": yp}
        return remote(part, part, h_sem.at[0, kind, q], h_sem.at[1, kind, q], where)

    def ret_copy(q, cc):
        part = res.at[q * 2 + cc]
        return remote(
            part, ret.at[ep], ret_sem.at[0, q * 2 + cc], ret_sem.at[1, ep], {"ep": q * 2 + cc}
        )

    def spread(q):
        t_copy(q, 0).start()
        t_copy(q, 1).start()

        @pl.when((q < z) & (z + 1 < nz))
        def _():
            z_copy(q, 1).start()

        @pl.when((q > z) & (z > 0))
        def _():
            z_copy(q, 0).start()

        sib_copy(q, t).start()

    def ranks_row(block):
        named = routes_all[block]
        mask = jnp.where((named[0:1] == ep) | (named[1:2] == ep), 1.0, 0.0)
        before = jnp.where(
            lax.broadcasted_iota(jnp.int32, (rows, rows), 0)
            < lax.broadcasted_iota(jnp.int32, (rows, rows), 1),
            1.0,
            0.0,
        ).astype(BF16)
        rank = jnp.dot(
            jnp.broadcast_to(mask, (8, rows)).astype(BF16), before, preferred_element_type=F32
        )[0:1]
        key = jnp.where(mask > 0.5, rank, -1.0)
        seat = lax.broadcasted_iota(jnp.int32, (cap, rows), 0).astype(F32)
        return jnp.where(seat == key, 1.0, 0.0).astype(BF16)

    def expert_in(q):
        for cc in range(2):
            pick = ranks_row(q * 2 + cc)
            parts = [
                jnp.dot(pick, tok[cc, q, k], preferred_element_type=F32) for k in range(4)
            ]
            square = sum(jnp.sum(part * part, axis=-1, keepdims=True) for part in parts)
            scale = lax.rsqrt(square * (1.0 / (4 * share)) + epsilon)
            for k in range(4):
                xs[pl.ds(cc * cap, cap), pl.ds(k * share, share)] = (
                    parts[k] * scale * gain_ref[:, pl.ds(k * share, share)]
                ).astype(BF16)

        tile = 256

        @pl.loop(0, gw.shape[1] // tile)
        def _(j):
            cols = pl.ds(pl.multiple_of(j * tile, tile), tile)
            g = jnp.dot(xs[...], gw[:, cols], preferred_element_type=F32)
            u = jnp.dot(xs[...], uw[:, cols], preferred_element_type=F32)
            hid[q, t, :, cols] = (jax.nn.silu(g) * u).astype(BF16)

        h_copy(q, 0).start()
        h_copy(q, 1).start()

    def expert_out(q):
        tile = 256
        span = hid.shape[3]

        @pl.loop(0, dw.shape[1] // tile)
        def _(j):
            cols = pl.ds(pl.multiple_of(j * tile, tile), tile)
            total = jnp.zeros((pair, tile), F32)
            for k in range(4):
                total = total + jnp.dot(
                    hid[q, k], dw[pl.ds(k * span, span), cols], preferred_element_type=F32
                )
            out = total.astype(BF16)
            res[q * 2, :, cols] = out[:cap]
            res[q * 2 + 1, :, cols] = out[cap:]

        for cc in range(2):
            mine = (q == z) & (c == cc)

            @pl.when(jnp.logical_not(mine))
            def _():
                ret_copy(q, cc).start()

            @pl.when(mine)
            def _():
                ret[ep] = res[q * 2 + cc]

    pad = xb.shape[0] - rows

    def halo_copy():
        return remote(
            xb.at[pl.ds(rows, pad)],
            xb.at[pl.ds(0, pad)],
            halo_sem.at[0],
            halo_sem.at[1],
            {"ep": ep + 1},
        )

    def ends_copy(by):
        return remote(
            ends.at[ep],
            ends.at[ep],
            ends_sem.at[0, by],
            ends_sem.at[1, ep],
            {"ep": (ep + by) % n_ep},
        )

    def project():
        for k in range(6, 9):
            loads[k].wait()
        strip = 64

        @pl.loop(0, rows // strip)
        def _(i):
            at = pl.ds(pl.multiple_of(i * strip, strip), strip)
            wide = mixv[at, :].astype(F32)
            scale = lax.rsqrt(jnp.mean(wide * wide, axis=-1, keepdims=True) + epsilon)
            xs[at, :] = (wide * scale * mix_gain_ref[...]).astype(BF16)

        tile = 256

        @pl.loop(0, wx.shape[1] // tile)
        def _(j):
            cols = pl.ds(pl.multiple_of(j * tile, tile), tile)
            xb[pl.ds(pad, rows), cols] = jnp.dot(
                xs[...], wx[:, cols], preferred_element_type=F32
            ).astype(BF16)
            yb[:, cols] = jnp.dot(xs[...], wy[:, cols], preferred_element_type=F32).astype(BF16)

        @pl.when(ep + 1 < n_ep)
        def _():
            halo_copy().start()

        @pl.when(ep == 0)
        def _():
            xb[pl.ds(0, pad), :] = jnp.zeros((pad, xb.shape[1]), BF16)

    def recur():
        for k in range(9, 12):
            loads[k].wait()

        @pl.when(ep > 0)
        def _():
            halo_copy().wait_recv()

        taps = taps_ref.shape[0]
        size = gaw.shape[1]
        for h in range(gaw.shape[0]):
            cols = pl.ds(h * size, size)
            wide = xb[:, cols].astype(F32)
            conv = jnp.zeros((rows, size), F32)
            for k in range(taps):
                first_row = pad - (taps - 1) + k
                conv = conv + taps_ref[k : k + 1, cols] * wide[first_row : first_row + rows]
            x_conv = conv.astype(BF16)
            gate_a = jnp.dot(x_conv, gaw[h], preferred_element_type=F32)
            gate_x = jnp.dot(x_conv, gxw[h], preferred_element_type=F32)
            log_decay = (
                -lru_scale * jax.nn.sigmoid(gate_a) * soft_ref[:, cols] + shiftv[:, cols]
            )
            av[:, cols] = jnp.exp(log_decay)
            bv[:, cols] = (
                jnp.sqrt(one_minus_exp(2.0 * log_decay))
                * jax.nn.sigmoid(gate_x)
                * x_conv.astype(F32)
            )
        width = av.shape[1]
        row = lax.broadcasted_iota(jnp.int32, (8, width), 0)

        def group(i, carry):
            at = pl.ds(pl.multiple_of(i * 8, 8), 8)
            a, b = av[at, :], bv[at, :]
            for by in (1, 2, 4):
                a_past, b_past = pltpu.roll(a, by, 0), pltpu.roll(b, by, 0)
                b = jnp.where(row >= by, a * b_past + b, b)
                a = jnp.where(row >= by, a * a_past, a)
            b = a * carry[1] + b
            a = a * carry[0]
            av[at, :] = a
            bv[at, :] = b
            return (a[7:8], b[7:8])

        through, state = lax.fori_loop(
            0, rows // 8, group, (jnp.ones((1, width), F32), jnp.zeros((1, width), F32))
        )
        ends[ep, 0:1] = through
        ends[ep, 1:2] = state
        for by in range(1, n_ep):
            ends_copy(by).start()

    def finish():
        carried = jnp.zeros((1, av.shape[1]), F32)
        for by in range(1, n_ep):
            other = (ep + by) % n_ep
            remote(
                ends.at[other], ends.at[other], ends_sem.at[0, 0], ends_sem.at[1, other], {"ep": other}
            ).wait_recv()
        for k in range(n_ep):
            entered = ends[k, 0:1] * carried + ends[k, 1:2]
            carried = jnp.where(k < ep, entered, carried)
        strip = 32

        @pl.loop(0, rows // strip)
        def _(i):
            at = pl.ds(pl.multiple_of(i * strip, strip), strip)
            state = bv[at, :] + av[at, :] * carried
            mix_ref[at, :] = (state * jax.nn.gelu(yb[at, :].astype(F32))).astype(BF16)

    for k in range(4):
        loads[k].wait()

    @pl.when(z + 1 < nz)
    def _():
        z_copy(z, 1).start()

    @pl.when(z > 0)
    def _():
        z_copy(z, 0).start()

    own_copy().start()
    for k in range(4, 6):
        loads[k].wait()
    for by in range(1, n_ep):
        other = (ep + by) % n_ep
        remote(
            rt_row, routes_all.at[other], rt_sem.at[0, 0], rt_sem.at[1, other], {"ep": other}
        ).wait_recv()
    remote(
        tok.at[1 - c, z], tok.at[1 - c, z], own_sem.at[0], own_sem.at[1], sibling
    ).wait_recv()
    expert_in(z)
    first = block_at(1)
    z_copy(first, 1).wait_recv()
    spread(first)

    def pass_hidden(q):
        h_copy(q, 0).wait_recv()
        h_copy(q, 3).start()
        h_copy(q, 1).wait_recv()
        h_copy(q, 2).start()

    project()
    pass_hidden(z)
    loads[12].wait()

    def step(s, carry):
        q = block_at(s)
        nxt = block_at(s + 1)
        far = block_at(s + 2)

        @pl.when(s + 1 == nz)
        def _():
            pass_hidden(q)

        @pl.when(s + 1 < nz)
        def _():
            t_copy(nxt, 0).wait_recv()
            t_copy(nxt, 3).start()
            sib_copy(nxt, xp).start()
            t_copy(nxt, 1).wait_recv()
            t_copy(nxt, 2).start()
            sib_copy(nxt, yp).start()

            @pl.when(s + 2 < nz)
            def _():
                z_copy(far, 1).wait_recv()
                spread(far)

            @pl.when(s > 0)
            def _():
                pass_hidden(q)

            t_copy(nxt, 2).wait_recv()
            t_copy(nxt, 3).wait_recv()
            sib_copy(nxt, dg).start()
            for k in range(4):
                sib_copy(nxt, k).wait_recv()
            expert_in(nxt)

        h_copy(q, 2).wait_recv()
        h_copy(q, 3).wait_recv()
        expert_out(q)

        @pl.when(s == 0)
        def _():
            recur()

        @pl.when(s == 1)
        def _():
            finish()

        return carry

    lax.fori_loop(0, nz, step, 0)

    one, two = rt_col[:, 0:1], rt_col[:, 1:2]
    lane = lax.broadcasted_iota(jnp.int32, (rows, 128), 1)
    mask = jnp.where((one == lane) | (two == lane), 1.0, 0.0)
    before = jnp.where(
        lax.broadcasted_iota(jnp.int32, (rows, rows), 1)
        < lax.broadcasted_iota(jnp.int32, (rows, rows), 0),
        1.0,
        0.0,
    ).astype(BF16)
    rank = jnp.dot(before, mask.astype(BF16), preferred_element_type=F32)
    key = jnp.where(mask > 0.5, rank, -1.0)
    total_weight = rw_col[:, 0:1] + rw_col[:, 1:2]
    part_one = rw_col[:, 0:1] / total_weight
    part_two = rw_col[:, 1:2] / total_weight
    seat = lax.broadcasted_iota(jnp.int32, (rows, cap), 1).astype(F32)
    for by in range(1, n_ep):
        other = (ep + by) % n_ep
        remote(
            res.at[other], ret.at[other], ret_sem.at[0, other], ret_sem.at[1, other], {"ep": other}
        ).wait_recv()
    total = jnp.zeros((rows, ret.shape[2]), F32)
    for e in range(n_ep):
        pick = jnp.where(seat == key[:, e : e + 1], 1.0, 0.0).astype(BF16)
        portion = jnp.where(one == e, part_one, 0.0) + jnp.where(two == e, part_two, 0.0)
        total = total + portion * jnp.dot(pick, ret[e], preferred_element_type=F32)
    out_ref[...] = total.astype(BF16)

    for by in range(1, n_ep):
        route_copy(by).wait_send()

    @pl.when(z + 1 < nz)
    def _():
        z_copy(z, 1).wait_send()

    @pl.when(z > 0)
    def _():
        z_copy(z, 0).wait_send()

    own_copy().wait_send()

    @pl.when(ep + 1 < n_ep)
    def _():
        halo_copy().wait_send()

    for by in range(1, n_ep):
        ends_copy(by).wait_send()

    def drain(q, carry):
        for kind in range(4):
            h_copy(q, kind).wait_send()

        @pl.when(q != z)
        def _():
            for kind in range(4):
                t_copy(q, kind).wait_send()
                sib_copy(q, kind).wait_send()

        @pl.when((q < z) & (z + 1 < nz))
        def _():
            z_copy(q, 1).wait_send()

        @pl.when((q > z) & (z > 0))
        def _():
            z_copy(q, 0).wait_send()

        for cc in range(2):

            @pl.when((q != z) | (c != cc))
            def _():
                ret_copy(q, cc).wait_send()

        return carry

    lax.fori_loop(0, nz, drain, 0)


def both_fused(
    mix_in,
    mix_gain,
    w_in_x,
    w_in_y,
    conv_taps,
    recur_gate_w,
    input_gate_w,
    decay_logit,
    decay_shift,
    moe_in,
    moe_gain,
    routes,
    route_weight,
    expert_gate,
    expert_up,
    expert_down,
):
    n_ep = lax.axis_size("ep")
    nz = n_ep // 2
    rows, features = moe_in.shape
    share = features // 4
    ff_dev, out_dev = expert_gate.shape[2], expert_down.shape[2]
    width = w_in_x.shape[1]
    cap = 2 * rows * routes.shape[1] // n_ep
    vmem = pl.BlockSpec(memory_space=pltpu.VMEM)
    hbm = pl.BlockSpec(memory_space=pltpu.HBM)
    dma = pltpu.SemaphoreType.DMA
    flops = 2 * n_ep * cap * features * (2 * ff_dev + out_dev)
    return pl.pallas_call(
        functools.partial(both_kernel, cap),
        out_shape=(
            jax.ShapeDtypeStruct((rows, width), BF16),
            jax.ShapeDtypeStruct((rows, out_dev), BF16),
        ),
        in_specs=[hbm] * 6 + [vmem] * 3 + [hbm] + [vmem] * 4 + [hbm] * 3,
        out_specs=(vmem, vmem),
        scratch_shapes=[
            pltpu.VMEM((2, nz, 4, rows, share), BF16),
            pltpu.VMEM((nz, 4, 2 * cap, ff_dev), BF16),
            pltpu.VMEM((2 * cap, features), BF16),
            pltpu.VMEM((n_ep, cap, out_dev), BF16),
            pltpu.VMEM((n_ep, cap, out_dev), BF16),
            pltpu.VMEM((n_ep, 2, rows), jnp.int32),
            pltpu.VMEM(expert_gate.shape[1:], BF16),
            pltpu.VMEM(expert_up.shape[1:], BF16),
            pltpu.VMEM(expert_down.shape[1:], BF16),
            dma((13,)),
            dma((2, n_ep)),
            dma((2, nz)),
            dma((nz,)),
            dma((2, 4, nz)),
            dma((2, 4, nz)),
            dma((2,)),
            dma((2, 4, nz)),
            dma((2, n_ep)),
            pltpu.VMEM(mix_in.shape, BF16),
            pltpu.VMEM(w_in_x.shape, BF16),
            pltpu.VMEM(w_in_y.shape, BF16),
            pltpu.VMEM(recur_gate_w.shape, BF16),
            pltpu.VMEM(input_gate_w.shape, BF16),
            pltpu.VMEM((rows, width), F32),
            pltpu.VMEM((16 + rows, width), BF16),
            pltpu.VMEM((rows, width), BF16),
            pltpu.VMEM((rows, width), F32),
            pltpu.VMEM((rows, width), F32),
            pltpu.VMEM((n_ep, 2, width), F32),
            dma((2,)),
            dma((2, n_ep)),
        ],
        compiler_params=pltpu.CompilerParams(
            collective_id=0, has_side_effects=True, vmem_limit_bytes=60 * 1024 * 1024
        ),
        cost_estimate=pl.CostEstimate(flops=flops, bytes_accessed=16 << 20, transcendentals=0),
        name="both",
    )(
        mix_in,
        w_in_x,
        w_in_y,
        recur_gate_w,
        input_gate_w,
        decay_shift,
        mix_gain[None, :],
        conv_taps,
        jax.nn.softplus(-decay_logit)[None, :],
        moe_in,
        moe_gain[None, :],
        routes.T,
        routes,
        route_weight,
        expert_gate,
        expert_up,
        expert_down,
    )


def from_behind(value, axis, by):
    count = lax.axis_size(axis)
    pairs = [(i, i + by) for i in range(count) if 0 <= i + by < count]
    return lax.ppermute(value, axis, pairs)


def entering(value, axis, combine, identity):
    count, index = (lax.axis_size(axis), lax.axis_index(axis))
    everything = jax.tree.map(lambda part: lax.all_gather(part, axis), value)
    start = jax.tree.map(
        lambda part, zero: jnp.broadcast_to(jnp.asarray(zero, part.dtype), part.shape),
        value,
        identity,
    )

    def hop(k, before):
        reached = k < index
        new = combine(before, jax.tree.map(lambda part: part[k], everything))
        return jax.tree.map(lambda a, b: jnp.where(reached, a, b), new, before)

    return lax.fori_loop(0, count, hop, start)


def norm_rows(rows, gain):
    widened = rows.astype(jnp.float32)
    scaled = widened * lax.rsqrt(jnp.mean(widened * widened, axis=-1, keepdims=True) + epsilon)
    return (scaled * gain[None, :]).astype(jnp.bfloat16)


def link(earlier, later):
    return (earlier[0] * later[0], later[0] * earlier[1] + later[1])


def fits_fused(moe_in, routes):
    n_ep = lax.axis_size("ep")
    gathered = n_ep * moe_in.size * moe_in.dtype.itemsize
    even = n_ep == 4 * routes.shape[1]
    return lax.axis_size("tp") == 4 and even and gathered <= (16 << 20)


def moe_staged(moe_in, moe_gain, routes, route_weight, expert_gate, expert_up, expert_down):
    moe_rows = norm_rows(moe_in, moe_gain)
    token_count = moe_rows.shape[0]
    feature_count = moe_rows.shape[1]
    choose_count = routes.shape[1]
    expert_count = lax.axis_size("ep")
    capacity = 2 * token_count * choose_count // expert_count
    slot_total = expert_count * capacity
    expert_ids = routes.reshape(-1)
    onehot = (expert_ids[:, None] == jnp.arange(expert_count, dtype=jnp.int32)[None, :]).astype(
        jnp.int32
    )
    slot_rank = jnp.sum(jnp.cumsum(onehot, axis=0) * onehot, axis=1) - 1
    slot_index = expert_ids * capacity + slot_rank
    token_index = jnp.repeat(jnp.arange(token_count, dtype=jnp.int32), choose_count)
    slot_owner = jnp.full((slot_total,), token_count, jnp.int32).at[slot_index].set(token_index)
    padded_rows = jnp.concatenate([moe_rows, jnp.zeros((1, feature_count), jnp.bfloat16)], axis=0)
    outgoing = padded_rows[slot_owner].reshape(expert_count, capacity, feature_count)
    column_width = feature_count // lax.axis_size("tp")
    own_columns = lax.dynamic_slice_in_dim(
        outgoing, lax.axis_index("tp") * column_width, column_width, 2
    )
    incoming = lax.all_to_all(own_columns, "ep", split_axis=0, concat_axis=0, tiled=True)
    piece = lax.all_gather(incoming, "tp", axis=2, tiled=True)
    flat_rows = piece.reshape(slot_total, piece.shape[2])
    gate_rows = expert_gate[0]
    up_rows = expert_up[0]
    gate_proj = jnp.dot(flat_rows, gate_rows, preferred_element_type=jnp.float32)
    up_proj = jnp.dot(flat_rows, up_rows, preferred_element_type=jnp.float32)
    hidden = (jax.nn.silu(gate_proj) * up_proj).astype(jnp.bfloat16)
    down_rows = expert_down[0]
    columns = jnp.dot(
        lax.all_gather(hidden, "tp", axis=1, tiled=True),
        down_rows,
        preferred_element_type=jnp.float32,
    )
    results = columns.astype(jnp.bfloat16).reshape(expert_count, capacity, expert_down.shape[2])
    returned = lax.all_to_all(results, "ep", split_axis=0, concat_axis=0, tiled=True).reshape(
        slot_total, expert_down.shape[2]
    )
    picked = (
        returned[slot_index]
        .astype(jnp.float32)
        .reshape(token_count, choose_count, expert_down.shape[2])
    )
    route_share = route_weight / jnp.sum(route_weight, axis=1, keepdims=True)
    moe_out = jnp.sum(route_share[:, :, None] * picked, axis=1).astype(jnp.bfloat16)
    return moe_out


def staged(
    mix_in,
    mix_gain,
    w_in_x,
    w_in_y,
    conv_taps,
    recur_gate_w,
    input_gate_w,
    decay_logit,
    decay_shift,
    moe_in,
    moe_gain,
    routes,
    route_weight,
    expert_gate,
    expert_up,
    expert_down,
):
    row_count = mix_in.shape[0]
    width_dev = w_in_x.shape[1]
    heads_dev = recur_gate_w.shape[0]
    block_size = recur_gate_w.shape[1]
    tap_count = conv_taps.shape[0]
    mixer_rows = norm_rows(mix_in, mix_gain)
    x_branch = jnp.dot(mixer_rows, w_in_x, preferred_element_type=jnp.float32).astype(jnp.bfloat16)
    y_branch = jnp.dot(mixer_rows, w_in_y, preferred_element_type=jnp.float32).astype(jnp.bfloat16)
    previous = from_behind(x_branch[row_count - (tap_count - 1) :], "ep", 1)
    padded = jnp.concatenate([previous, x_branch], axis=0)
    conv_sum = jnp.zeros((row_count, width_dev), jnp.float32)
    for tap_index in range(tap_count):
        conv_sum = conv_sum + conv_taps[tap_index][None, :] * padded[
            tap_index : tap_index + row_count
        ].astype(jnp.float32)
    x_conv = conv_sum.astype(jnp.bfloat16)
    heads_in = x_conv.reshape(row_count, heads_dev, block_size)
    gate_a = jnp.einsum(
        "thi,hij->thj", heads_in, recur_gate_w, preferred_element_type=jnp.float32
    ).reshape(row_count, width_dev)
    gate_x = jnp.einsum(
        "thi,hij->thj", heads_in, input_gate_w, preferred_element_type=jnp.float32
    ).reshape(row_count, width_dev)
    log_decay = (
        -lru_scale * jax.nn.sigmoid(gate_a) * jax.nn.softplus(-decay_logit)[None, :] + decay_shift
    )
    lru_drive = (
        jnp.sqrt(-jnp.expm1(2.0 * log_decay)) * jax.nn.sigmoid(gate_x) * x_conv.astype(jnp.float32)
    )
    through, local_state = lax.associative_scan(link, (jnp.exp(log_decay), lru_drive), axis=0)
    identity = (jnp.ones((width_dev,), jnp.float32), jnp.zeros((width_dev,), jnp.float32))
    carried = entering((through[row_count - 1], local_state[row_count - 1]), "ep", link, identity)
    lru_state = local_state + through * carried[1][None, :]
    mixer_out = (lru_state * jax.nn.gelu(y_branch.astype(jnp.float32))).astype(jnp.bfloat16)
    moe_out = moe_staged(
        moe_in, moe_gain, routes, route_weight, expert_gate, expert_up, expert_down
    )
    return (mixer_out, moe_out)


def local(*args):
    return (both_fused if fits_fused(args[9], args[11]) else staged)(*args)


def solution(mesh):
    placed = (
        P("ep", None),
        P(),
        P(None, "tp"),
        P(None, "tp"),
        P(None, "tp"),
        P("tp", None, None),
        P("tp", None, None),
        P("tp"),
        P("ep", "tp"),
        P("ep", None),
        P(),
        P("ep", None),
        P("ep", None),
        P("ep", None, "tp"),
        P("ep", None, "tp"),
        P("ep", None, "tp"),
    )
    return jax.shard_map(
        local, mesh=mesh, in_specs=placed, out_specs=(P("ep", "tp"), P("ep", "tp")), check_vma=False
    )
```

```python
import functools

import jax
import jax.numpy as jnp
from jax import lax
from jax.experimental import pallas as pl
from jax.experimental.pallas import tpu as pltpu
from jax.sharding import PartitionSpec as P

epsilon = 1e-06
lru_scale = 8.0
MESH = pl.DeviceIdType.MESH
F32 = jnp.float32
BF16 = jnp.bfloat16


block_order = ((0, 2, 3, 1), (1, 2, 3, 0), (2, 1, 0, 3), (3, 1, 0, 2))


def one_minus_exp(value):
    series = jnp.full_like(value, 1.0 / 9.0)
    for k in range(8, 1, -1):
        series = (1.0 + value * series) * (1.0 / k)
    series = 1.0 + value * series
    return jnp.where(value > -0.5, -value * series, 1.0 - jnp.exp(value))


def both_kernel(
    cap,
    mix_hbm,
    wx_hbm,
    wy_hbm,
    ga_hbm,
    gx_hbm,
    shift_hbm,
    mix_gain_ref,
    taps_ref,
    soft_ref,
    moe_hbm,
    gain_ref,
    rt_row,
    rw_row,
    gate_hbm,
    up_hbm,
    down_hbm,
    mix_ref,
    out_ref,
    tok,
    hid,
    xs,
    res,
    ret,
    routes_all,
    gw,
    uw,
    dw,
    load_sem,
    rt_sem,
    z_send,
    z_recv,
    t_sem,
    sib_sem,
    own_sem,
    h_sem,
    ret_sem,
    mixv,
    wx,
    wy,
    gaw,
    gxw,
    shiftv,
    xb,
    yb,
    av,
    bv,
    ends,
    halo_sem,
    ends_sem,
):
    n_ep = lax.axis_size("ep")
    nz = n_ep // 2
    ep = lax.axis_index("ep")
    t = lax.axis_index("tp")
    z, c = ep // 2, ep % 2
    y, x = t // 2, t % 2
    xp, yp, dg = y * 2 + (1 - x), (1 - y) * 2 + x, 3 - t
    rows, share = tok.shape[3], tok.shape[4]
    half = rows // 2
    pair = 2 * cap
    pair_half = pair // 2
    sibling = {"ep": z * 2 + (1 - c)}
    table = block_order

    def block_at(s):
        q = jnp.int32(0)
        for zz in range(nz):
            for ss in range(nz):
                q = jnp.where((z == zz) & (s == ss), table[zz][ss], q)
        return q

    def remote(src, dst, send, recv, where):
        return pltpu.make_async_remote_copy(
            src_ref=src,
            dst_ref=dst,
            send_sem=send,
            recv_sem=recv,
            device_id=where,
            device_id_type=MESH,
        )

    loads = [
        pltpu.make_async_copy(
            moe_hbm.at[:, pl.ds(k * share, share)], tok.at[c, z, k], load_sem.at[k]
        )
        for k in range(4)
    ] + [
        pltpu.make_async_copy(gate_hbm.at[0], gw, load_sem.at[4]),
        pltpu.make_async_copy(up_hbm.at[0], uw, load_sem.at[5]),
        pltpu.make_async_copy(mix_hbm, mixv, load_sem.at[6]),
        pltpu.make_async_copy(wx_hbm, wx, load_sem.at[7]),
        pltpu.make_async_copy(wy_hbm, wy, load_sem.at[8]),
        pltpu.make_async_copy(ga_hbm, gaw, load_sem.at[9]),
        pltpu.make_async_copy(gx_hbm, gxw, load_sem.at[10]),
        pltpu.make_async_copy(shift_hbm, shiftv, load_sem.at[11]),
        pltpu.make_async_copy(down_hbm.at[0], dw, load_sem.at[12]),
    ]
    for copy in loads:
        copy.start()

    barrier = pltpu.get_barrier_semaphore()
    for by in range(1, n_ep):
        pl.semaphore_signal(
            barrier, inc=1, device_id={"ep": (ep + by) % n_ep}, device_id_type=MESH
        )
    for peer in (xp, yp):
        pl.semaphore_signal(barrier, inc=1, device_id={"tp": peer}, device_id_type=MESH)
    pl.semaphore_wait(barrier, n_ep + 1)

    def route_copy(by):
        return remote(
            rt_row,
            routes_all.at[ep],
            rt_sem.at[0, by],
            rt_sem.at[1, ep],
            {"ep": (ep + by) % n_ep},
        )

    for by in range(1, n_ep):
        route_copy(by).start()
    routes_all[ep] = rt_row[...]

    def z_copy(q, up):
        return remote(
            tok.at[c, q, t],
            tok.at[c, q, t],
            z_send.at[up, q],
            z_recv.at[q],
            {"ep": ep + (2 if up else -2)},
        )

    def t_copy(q, kind):
        owner = (t, t, t, t, yp, xp)[kind]
        start = (0, half, half, 0, half, 0)[kind]
        part = tok.at[c, q, owner, pl.ds(start, half)]
        where = {"tp": (xp, yp)[kind % 2]}
        return remote(part, part, t_sem.at[0, kind, q], t_sem.at[1, kind, q], where)

    def sib_copy(q, k):
        part = tok.at[c, q, k]
        return remote(part, part, sib_sem.at[0, k, q], sib_sem.at[1, k, q], sibling)

    def own_copy():
        part = tok.at[c, z]
        return remote(part, part, own_sem.at[0], own_sem.at[1], sibling)

    def h_copy(q, kind):
        owner = (t, t, t, t, yp, xp)[kind]
        start = (0, pair_half, pair_half, 0, pair_half, 0)[kind]
        part = hid.at[q, owner, pl.ds(start, pair_half)]
        where = {"tp": (xp, yp)[kind % 2]}
        return remote(part, part, h_sem.at[0, kind, q], h_sem.at[1, kind, q], where)

    def ret_copy(q, cc):
        part = res.at[q * 2 + cc]
        return remote(
            part, ret.at[ep], ret_sem.at[0, q * 2 + cc], ret_sem.at[1, ep], {"ep": q * 2 + cc}
        )

    def spread(q):
        for kind in range(4):
            t_copy(q, kind).start()
        sib_copy(q, t).start()

    def arrive(q):
        z_copy(q, 1).wait_recv()

        @pl.when((q < z) & (z + 1 < nz))
        def _():
            z_copy(q, 1).start()

        @pl.when((q > z) & (z > 0))
        def _():
            z_copy(q, 0).start()

    def ranks_row(block):
        named = routes_all[block]
        mask = jnp.where((named[0:1] == ep) | (named[1:2] == ep), 1.0, 0.0)
        before = jnp.where(
            lax.broadcasted_iota(jnp.int32, (rows, rows), 0)
            < lax.broadcasted_iota(jnp.int32, (rows, rows), 1),
            1.0,
            0.0,
        ).astype(BF16)
        rank = jnp.dot(
            jnp.broadcast_to(mask, (8, rows)).astype(BF16), before, preferred_element_type=F32
        )[0:1]
        key = jnp.where(mask > 0.5, rank, -1.0)
        seat = lax.broadcasted_iota(jnp.int32, (cap, rows), 0).astype(F32)
        return jnp.where(seat == key, 1.0, 0.0).astype(BF16)

    def expert_in(q):
        for cc in range(2):
            pick = ranks_row(q * 2 + cc)
            parts = [
                jnp.dot(pick, tok[cc, q, k], preferred_element_type=F32) for k in range(4)
            ]
            square = sum(jnp.sum(part * part, axis=-1, keepdims=True) for part in parts)
            scale = lax.rsqrt(square * (1.0 / (4 * share)) + epsilon)
            for k in range(4):
                xs[pl.ds(cc * cap, cap), pl.ds(k * share, share)] = (
                    parts[k] * scale * gain_ref[:, pl.ds(k * share, share)]
                ).astype(BF16)

        tile = 256

        @pl.loop(0, gw.shape[1] // tile)
        def _(j):
            cols = pl.ds(pl.multiple_of(j * tile, tile), tile)
            g = jnp.dot(xs[...], gw[:, cols], preferred_element_type=F32)
            u = jnp.dot(xs[...], uw[:, cols], preferred_element_type=F32)
            hid[q, t, :, cols] = (jax.nn.silu(g) * u).astype(BF16)

        for kind in range(4):
            h_copy(q, kind).start()

    def expert_out(q):
        tile = 256
        span = hid.shape[3]

        @pl.loop(0, dw.shape[1] // tile)
        def _(j):
            cols = pl.ds(pl.multiple_of(j * tile, tile), tile)
            total = jnp.zeros((pair, tile), F32)
            for k in range(4):
                total = total + jnp.dot(
                    hid[q, k], dw[pl.ds(k * span, span), cols], preferred_element_type=F32
                )
            out = total.astype(BF16)
            res[q * 2, :, cols] = out[:cap]
            res[q * 2 + 1, :, cols] = out[cap:]

        for cc in range(2):
            mine = (q == z) & (c == cc)

            @pl.when(jnp.logical_not(mine))
            def _():
                ret_copy(q, cc).start()

            @pl.when(mine)
            def _():
                ret[ep] = res[q * 2 + cc]

    pad = xb.shape[0] - rows

    def halo_copy():
        return remote(
            xb.at[pl.ds(rows, pad)],
            xb.at[pl.ds(0, pad)],
            halo_sem.at[0],
            halo_sem.at[1],
            {"ep": ep + 1},
        )

    def ends_copy(by):
        return remote(
            ends.at[ep],
            ends.at[ep],
            ends_sem.at[0, by],
            ends_sem.at[1, ep],
            {"ep": (ep + by) % n_ep},
        )

    def project():
        for k in range(6, 9):
            loads[k].wait()
        strip = 64

        @pl.loop(0, rows // strip)
        def _(i):
            at = pl.ds(pl.multiple_of(i * strip, strip), strip)
            wide = mixv[at, :].astype(F32)
            scale = lax.rsqrt(jnp.mean(wide * wide, axis=-1, keepdims=True) + epsilon)
            xs[at, :] = (wide * scale * mix_gain_ref[...]).astype(BF16)

        tile = 256

        @pl.loop(0, wx.shape[1] // tile)
        def _(j):
            cols = pl.ds(pl.multiple_of(j * tile, tile), tile)
            xb[pl.ds(pad, rows), cols] = jnp.dot(
                xs[...], wx[:, cols], preferred_element_type=F32
            ).astype(BF16)
            yb[:, cols] = jnp.dot(xs[...], wy[:, cols], preferred_element_type=F32).astype(BF16)

        @pl.when(ep + 1 < n_ep)
        def _():
            halo_copy().start()

        @pl.when(ep == 0)
        def _():
            xb[pl.ds(0, pad), :] = jnp.zeros((pad, xb.shape[1]), BF16)

    def drives():
        for k in range(9, 12):
            loads[k].wait()

        @pl.when(ep > 0)
        def _():
            halo_copy().wait_recv()

        taps = taps_ref.shape[0]
        size = gaw.shape[1]
        for h in range(gaw.shape[0]):
            cols = pl.ds(h * size, size)
            wide = xb[:, cols].astype(F32)
            conv = jnp.zeros((rows, size), F32)
            for k in range(taps):
                first_row = pad - (taps - 1) + k
                conv = conv + taps_ref[k : k + 1, cols] * wide[first_row : first_row + rows]
            x_conv = conv.astype(BF16)
            gate_a = jnp.dot(x_conv, gaw[h], preferred_element_type=F32)
            gate_x = jnp.dot(x_conv, gxw[h], preferred_element_type=F32)
            log_decay = (
                -lru_scale * jax.nn.sigmoid(gate_a) * soft_ref[:, cols] + shiftv[:, cols]
            )
            av[:, cols] = jnp.exp(log_decay)
            bv[:, cols] = (
                jnp.sqrt(one_minus_exp(2.0 * log_decay))
                * jax.nn.sigmoid(gate_x)
                * x_conv.astype(F32)
            )

    def recur():
        width = av.shape[1]
        row = lax.broadcasted_iota(jnp.int32, (8, width), 0)

        def group(i, carry):
            at = pl.ds(pl.multiple_of(i * 8, 8), 8)
            a, b = av[at, :], bv[at, :]
            for by in (1, 2, 4):
                a_past, b_past = pltpu.roll(a, by, 0), pltpu.roll(b, by, 0)
                b = jnp.where(row >= by, a * b_past + b, b)
                a = jnp.where(row >= by, a * a_past, a)
            b = a * carry[1] + b
            a = a * carry[0]
            av[at, :] = a
            bv[at, :] = b
            return (a[7:8], b[7:8])

        through, state = lax.fori_loop(
            0, rows // 8, group, (jnp.ones((1, width), F32), jnp.zeros((1, width), F32))
        )
        ends[ep, 0:1] = through
        ends[ep, 1:2] = state
        for by in range(1, n_ep):
            ends_copy(by).start()

    def finish():
        carried = jnp.zeros((1, av.shape[1]), F32)
        for by in range(1, n_ep):
            other = (ep + by) % n_ep
            remote(
                ends.at[other], ends.at[other], ends_sem.at[0, 0], ends_sem.at[1, other], {"ep": other}
            ).wait_recv()
        for k in range(n_ep):
            entered = ends[k, 0:1] * carried + ends[k, 1:2]
            carried = jnp.where(k < ep, entered, carried)
        strip = 32

        @pl.loop(0, rows // strip)
        def _(i):
            at = pl.ds(pl.multiple_of(i * strip, strip), strip)
            state = bv[at, :] + av[at, :] * carried
            mix_ref[at, :] = (state * jax.nn.gelu(yb[at, :].astype(F32))).astype(BF16)

    for k in range(4):
        loads[k].wait()

    @pl.when(z + 1 < nz)
    def _():
        z_copy(z, 1).start()

    @pl.when(z > 0)
    def _():
        z_copy(z, 0).start()

    own_copy().start()
    for k in range(4, 6):
        loads[k].wait()
    for by in range(1, n_ep):
        other = (ep + by) % n_ep
        remote(
            rt_row, routes_all.at[other], rt_sem.at[0, 0], rt_sem.at[1, other], {"ep": other}
        ).wait_recv()
    remote(
        tok.at[1 - c, z], tok.at[1 - c, z], own_sem.at[0], own_sem.at[1], sibling
    ).wait_recv()
    expert_in(z)
    first = block_at(1)

    @pl.when(z > 0)
    def _():
        arrive(z - 1)

    @pl.when(z + 1 < nz)
    def _():
        arrive(z + 1)

    @pl.when((first == z + 2) | (first == z - 2))
    def _():
        arrive(first)

    spread(first)

    def pass_hidden(q):
        h_copy(q, 0).wait_recv()
        h_copy(q, 5).start()
        h_copy(q, 1).wait_recv()
        h_copy(q, 4).start()

    project()
    pass_hidden(z)
    loads[12].wait()

    @pl.when((z > 0) & (z + 1 < nz))
    def _():
        arrive(jnp.where(z + 2 < nz, z + 2, z - 2))

    def step(s, carry):
        q = block_at(s)
        nxt = block_at(s + 1)
        far = block_at(s + 2)

        @pl.when(s + 1 == nz)
        def _():
            pass_hidden(q)

        @pl.when(s + 1 < nz)
        def _():
            t_copy(nxt, 0).wait_recv()
            t_copy(nxt, 5).start()
            t_copy(nxt, 1).wait_recv()
            t_copy(nxt, 4).start()

            @pl.when(s + 2 < nz)
            def _():
                @pl.when((far == z + 3) | (far == z - 3))
                def _():
                    arrive(far)

                spread(far)

            @pl.when(s > 0)
            def _():
                pass_hidden(q)

            t_copy(nxt, 2).wait_recv()
            sib_copy(nxt, xp).start()
            t_copy(nxt, 3).wait_recv()
            sib_copy(nxt, yp).start()
            t_copy(nxt, 4).wait_recv()
            t_copy(nxt, 5).wait_recv()
            sib_copy(nxt, dg).start()
            for k in range(4):
                sib_copy(nxt, k).wait_recv()
            expert_in(nxt)

        for kind in range(2, 6):
            h_copy(q, kind).wait_recv()
        expert_out(q)

        @pl.when(s == 0)
        def _():
            drives()

        @pl.when(s == 1)
        def _():
            recur()

        @pl.when(s == 2)
        def _():
            finish()

        return carry

    lax.fori_loop(0, nz, step, 0)

    weights = rw_row[...]
    columns = jnp.concatenate(
        [
            rt_row[...].astype(F32),
            weights / (weights[0:1] + weights[1:2]),
            jnp.zeros((124, rows), F32),
        ],
        axis=0,
    ).T
    one, two = columns[:, 0:1].astype(jnp.int32), columns[:, 1:2].astype(jnp.int32)
    lane = lax.broadcasted_iota(jnp.int32, (rows, 128), 1)
    mask = jnp.where((one == lane) | (two == lane), 1.0, 0.0)
    before = jnp.where(
        lax.broadcasted_iota(jnp.int32, (rows, rows), 1)
        < lax.broadcasted_iota(jnp.int32, (rows, rows), 0),
        1.0,
        0.0,
    ).astype(BF16)
    rank = jnp.dot(before, mask.astype(BF16), preferred_element_type=F32)
    key = jnp.where(mask > 0.5, rank, -1.0)
    part_one, part_two = columns[:, 2:3], columns[:, 3:4]
    seat = lax.broadcasted_iota(jnp.int32, (rows, cap), 1).astype(F32)
    for by in range(1, n_ep):
        other = (ep + by) % n_ep
        remote(
            res.at[other], ret.at[other], ret_sem.at[0, other], ret_sem.at[1, other], {"ep": other}
        ).wait_recv()
    total = jnp.zeros((rows, ret.shape[2]), F32)
    for e in range(n_ep):
        pick = jnp.where(seat == key[:, e : e + 1], 1.0, 0.0).astype(BF16)
        portion = jnp.where(one == e, part_one, 0.0) + jnp.where(two == e, part_two, 0.0)
        total = total + portion * jnp.dot(pick, ret[e], preferred_element_type=F32)
    out_ref[...] = total.astype(BF16)

    for by in range(1, n_ep):
        route_copy(by).wait_send()

    @pl.when(z + 1 < nz)
    def _():
        z_copy(z, 1).wait_send()

    @pl.when(z > 0)
    def _():
        z_copy(z, 0).wait_send()

    own_copy().wait_send()

    @pl.when(ep + 1 < n_ep)
    def _():
        halo_copy().wait_send()

    for by in range(1, n_ep):
        ends_copy(by).wait_send()

    def drain(q, carry):
        for kind in range(6):
            h_copy(q, kind).wait_send()

        @pl.when(q != z)
        def _():
            for kind in range(6):
                t_copy(q, kind).wait_send()
            for k in range(4):
                sib_copy(q, k).wait_send()

        @pl.when((q < z) & (z + 1 < nz))
        def _():
            z_copy(q, 1).wait_send()

        @pl.when((q > z) & (z > 0))
        def _():
            z_copy(q, 0).wait_send()

        for cc in range(2):

            @pl.when((q != z) | (c != cc))
            def _():
                ret_copy(q, cc).wait_send()

        return carry

    lax.fori_loop(0, nz, drain, 0)


def both_fused(
    mix_in,
    mix_gain,
    w_in_x,
    w_in_y,
    conv_taps,
    recur_gate_w,
    input_gate_w,
    decay_logit,
    decay_shift,
    moe_in,
    moe_gain,
    routes,
    route_weight,
    expert_gate,
    expert_up,
    expert_down,
):
    n_ep = lax.axis_size("ep")
    nz = n_ep // 2
    rows, features = moe_in.shape
    share = features // 4
    ff_dev, out_dev = expert_gate.shape[2], expert_down.shape[2]
    width = w_in_x.shape[1]
    cap = 2 * rows * routes.shape[1] // n_ep
    vmem = pl.BlockSpec(memory_space=pltpu.VMEM)
    hbm = pl.BlockSpec(memory_space=pltpu.HBM)
    dma = pltpu.SemaphoreType.DMA
    flops = 2 * n_ep * cap * features * (2 * ff_dev + out_dev)
    return pl.pallas_call(
        functools.partial(both_kernel, cap),
        out_shape=(
            jax.ShapeDtypeStruct((rows, width), BF16),
            jax.ShapeDtypeStruct((rows, out_dev), BF16),
        ),
        in_specs=[hbm] * 6 + [vmem] * 3 + [hbm] + [vmem] * 3 + [hbm] * 3,
        out_specs=(vmem, vmem),
        scratch_shapes=[
            pltpu.VMEM((2, nz, 4, rows, share), BF16),
            pltpu.VMEM((nz, 4, 2 * cap, ff_dev), BF16),
            pltpu.VMEM((2 * cap, features), BF16),
            pltpu.VMEM((n_ep, cap, out_dev), BF16),
            pltpu.VMEM((n_ep, cap, out_dev), BF16),
            pltpu.VMEM((n_ep, 2, rows), jnp.int32),
            pltpu.VMEM(expert_gate.shape[1:], BF16),
            pltpu.VMEM(expert_up.shape[1:], BF16),
            pltpu.VMEM(expert_down.shape[1:], BF16),
            dma((13,)),
            dma((2, n_ep)),
            dma((2, nz)),
            dma((nz,)),
            dma((2, 6, nz)),
            dma((2, 4, nz)),
            dma((2,)),
            dma((2, 6, nz)),
            dma((2, n_ep)),
            pltpu.VMEM(mix_in.shape, BF16),
            pltpu.VMEM(w_in_x.shape, BF16),
            pltpu.VMEM(w_in_y.shape, BF16),
            pltpu.VMEM(recur_gate_w.shape, BF16),
            pltpu.VMEM(input_gate_w.shape, BF16),
            pltpu.VMEM((rows, width), F32),
            pltpu.VMEM((16 + rows, width), BF16),
            pltpu.VMEM((rows, width), BF16),
            pltpu.VMEM((rows, width), F32),
            pltpu.VMEM((rows, width), F32),
            pltpu.VMEM((n_ep, 2, width), F32),
            dma((2,)),
            dma((2, n_ep)),
        ],
        compiler_params=pltpu.CompilerParams(
            collective_id=0, has_side_effects=True, vmem_limit_bytes=60 * 1024 * 1024
        ),
        cost_estimate=pl.CostEstimate(flops=flops, bytes_accessed=16 << 20, transcendentals=0),
        name="both",
    )(
        mix_in,
        w_in_x,
        w_in_y,
        recur_gate_w,
        input_gate_w,
        decay_shift,
        mix_gain[None, :],
        conv_taps,
        jax.nn.softplus(-decay_logit)[None, :],
        moe_in,
        moe_gain[None, :],
        routes.T,
        route_weight.T,
        expert_gate,
        expert_up,
        expert_down,
    )


def from_behind(value, axis, by):
    count = lax.axis_size(axis)
    pairs = [(i, i + by) for i in range(count) if 0 <= i + by < count]
    return lax.ppermute(value, axis, pairs)


def entering(value, axis, combine, identity):
    count, index = (lax.axis_size(axis), lax.axis_index(axis))
    everything = jax.tree.map(lambda part: lax.all_gather(part, axis), value)
    start = jax.tree.map(
        lambda part, zero: jnp.broadcast_to(jnp.asarray(zero, part.dtype), part.shape),
        value,
        identity,
    )

    def hop(k, before):
        reached = k < index
        new = combine(before, jax.tree.map(lambda part: part[k], everything))
        return jax.tree.map(lambda a, b: jnp.where(reached, a, b), new, before)

    return lax.fori_loop(0, count, hop, start)


def norm_rows(rows, gain):
    widened = rows.astype(jnp.float32)
    scaled = widened * lax.rsqrt(jnp.mean(widened * widened, axis=-1, keepdims=True) + epsilon)
    return (scaled * gain[None, :]).astype(jnp.bfloat16)


def link(earlier, later):
    return (earlier[0] * later[0], later[0] * earlier[1] + later[1])


def fits_fused(moe_in, routes):
    n_ep = lax.axis_size("ep")
    gathered = n_ep * moe_in.size * moe_in.dtype.itemsize
    even = n_ep == 4 * routes.shape[1] == 2 * len(block_order)
    return lax.axis_size("tp") == 4 and even and gathered <= (16 << 20)


def moe_staged(moe_in, moe_gain, routes, route_weight, expert_gate, expert_up, expert_down):
    moe_rows = norm_rows(moe_in, moe_gain)
    token_count = moe_rows.shape[0]
    feature_count = moe_rows.shape[1]
    choose_count = routes.shape[1]
    expert_count = lax.axis_size("ep")
    capacity = 2 * token_count * choose_count // expert_count
    slot_total = expert_count * capacity
    expert_ids = routes.reshape(-1)
    onehot = (expert_ids[:, None] == jnp.arange(expert_count, dtype=jnp.int32)[None, :]).astype(
        jnp.int32
    )
    slot_rank = jnp.sum(jnp.cumsum(onehot, axis=0) * onehot, axis=1) - 1
    slot_index = expert_ids * capacity + slot_rank
    token_index = jnp.repeat(jnp.arange(token_count, dtype=jnp.int32), choose_count)
    slot_owner = jnp.full((slot_total,), token_count, jnp.int32).at[slot_index].set(token_index)
    padded_rows = jnp.concatenate([moe_rows, jnp.zeros((1, feature_count), jnp.bfloat16)], axis=0)
    outgoing = padded_rows[slot_owner].reshape(expert_count, capacity, feature_count)
    column_width = feature_count // lax.axis_size("tp")
    own_columns = lax.dynamic_slice_in_dim(
        outgoing, lax.axis_index("tp") * column_width, column_width, 2
    )
    incoming = lax.all_to_all(own_columns, "ep", split_axis=0, concat_axis=0, tiled=True)
    piece = lax.all_gather(incoming, "tp", axis=2, tiled=True)
    flat_rows = piece.reshape(slot_total, piece.shape[2])
    gate_rows = expert_gate[0]
    up_rows = expert_up[0]
    gate_proj = jnp.dot(flat_rows, gate_rows, preferred_element_type=jnp.float32)
    up_proj = jnp.dot(flat_rows, up_rows, preferred_element_type=jnp.float32)
    hidden = (jax.nn.silu(gate_proj) * up_proj).astype(jnp.bfloat16)
    down_rows = expert_down[0]
    columns = jnp.dot(
        lax.all_gather(hidden, "tp", axis=1, tiled=True),
        down_rows,
        preferred_element_type=jnp.float32,
    )
    results = columns.astype(jnp.bfloat16).reshape(expert_count, capacity, expert_down.shape[2])
    returned = lax.all_to_all(results, "ep", split_axis=0, concat_axis=0, tiled=True).reshape(
        slot_total, expert_down.shape[2]
    )
    picked = (
        returned[slot_index]
        .astype(jnp.float32)
        .reshape(token_count, choose_count, expert_down.shape[2])
    )
    route_share = route_weight / jnp.sum(route_weight, axis=1, keepdims=True)
    moe_out = jnp.sum(route_share[:, :, None] * picked, axis=1).astype(jnp.bfloat16)
    return moe_out


def staged(
    mix_in,
    mix_gain,
    w_in_x,
    w_in_y,
    conv_taps,
    recur_gate_w,
    input_gate_w,
    decay_logit,
    decay_shift,
    moe_in,
    moe_gain,
    routes,
    route_weight,
    expert_gate,
    expert_up,
    expert_down,
):
    row_count = mix_in.shape[0]
    width_dev = w_in_x.shape[1]
    heads_dev = recur_gate_w.shape[0]
    block_size = recur_gate_w.shape[1]
    tap_count = conv_taps.shape[0]
    mixer_rows = norm_rows(mix_in, mix_gain)
    x_branch = jnp.dot(mixer_rows, w_in_x, preferred_element_type=jnp.float32).astype(jnp.bfloat16)
    y_branch = jnp.dot(mixer_rows, w_in_y, preferred_element_type=jnp.float32).astype(jnp.bfloat16)
    previous = from_behind(x_branch[row_count - (tap_count - 1) :], "ep", 1)
    padded = jnp.concatenate([previous, x_branch], axis=0)
    conv_sum = jnp.zeros((row_count, width_dev), jnp.float32)
    for tap_index in range(tap_count):
        conv_sum = conv_sum + conv_taps[tap_index][None, :] * padded[
            tap_index : tap_index + row_count
        ].astype(jnp.float32)
    x_conv = conv_sum.astype(jnp.bfloat16)
    heads_in = x_conv.reshape(row_count, heads_dev, block_size)
    gate_a = jnp.einsum(
        "thi,hij->thj", heads_in, recur_gate_w, preferred_element_type=jnp.float32
    ).reshape(row_count, width_dev)
    gate_x = jnp.einsum(
        "thi,hij->thj", heads_in, input_gate_w, preferred_element_type=jnp.float32
    ).reshape(row_count, width_dev)
    log_decay = (
        -lru_scale * jax.nn.sigmoid(gate_a) * jax.nn.softplus(-decay_logit)[None, :] + decay_shift
    )
    lru_drive = (
        jnp.sqrt(-jnp.expm1(2.0 * log_decay)) * jax.nn.sigmoid(gate_x) * x_conv.astype(jnp.float32)
    )
    through, local_state = lax.associative_scan(link, (jnp.exp(log_decay), lru_drive), axis=0)
    identity = (jnp.ones((width_dev,), jnp.float32), jnp.zeros((width_dev,), jnp.float32))
    carried = entering((through[row_count - 1], local_state[row_count - 1]), "ep", link, identity)
    lru_state = local_state + through * carried[1][None, :]
    mixer_out = (lru_state * jax.nn.gelu(y_branch.astype(jnp.float32))).astype(jnp.bfloat16)
    moe_out = moe_staged(
        moe_in, moe_gain, routes, route_weight, expert_gate, expert_up, expert_down
    )
    return (mixer_out, moe_out)


def local(*args):
    return (both_fused if fits_fused(args[9], args[11]) else staged)(*args)


def solution(mesh):
    placed = (
        P("ep", None),
        P(),
        P(None, "tp"),
        P(None, "tp"),
        P(None, "tp"),
        P("tp", None, None),
        P("tp", None, None),
        P("tp"),
        P("ep", "tp"),
        P("ep", None),
        P(),
        P("ep", None),
        P("ep", None),
        P("ep", None, "tp"),
        P("ep", None, "tp"),
        P("ep", None, "tp"),
    )
    return jax.shard_map(
        local, mesh=mesh, in_specs=placed, out_specs=(P("ep", "tp"), P("ep", "tp")), check_vma=False
    )
```
